32 devices in a mesh: grp: 2 (over y), sp: 4 (over z), tp: 4 (over x, core).
Axes of the slice: x: 2, y: 2, z: 4, core: 2. Of those that a mesh axis runs over, the one named last changes fastest.
Arguments:
- stream: bfloat16 [2048, 2048], P(('grp', 'sp')), parts along dimension 0, may hold values from -6 to 6
- doc_ids: int32 [2048], P(('grp', 'sp')), parts along dimension 0, may hold values from 0 to 1, never falling along the last dimension, each value on 1 to 768 neighbouring positions
- norm_gain: float32 [2, 2048], replicated, may hold values from 0.1 to 1.9
- query_weight: bfloat16 [2, 2048, 1024], P(None, 'sp', 'tp'), may hold values from -0.125 to 0.125
- key_weight: bfloat16 [2, 2048, 1024], P(None, 'sp', 'tp'), may hold values from -0.125 to 0.125
- value_weight: bfloat16 [2, 2048, 1024], P(None, 'sp', 'tp'), may hold values from -0.125 to 0.125
- out_weight: bfloat16 [2, 1024, 2048], P(None, 'sp', 'tp'), may hold values from -0.75 to 0.75
- query_gain: float32 [2, 64], replicated, may hold values from 0.1 to 1.9
- key_gain: float32 [2, 64], replicated, may hold values from 0.1 to 1.9
- rel_bias: float32 [16, 513], P('tp'), may hold values from -4 to 250
Outputs:
- encoded: bfloat16 [2048, 2048], P(('grp', 'sp')), parts along dimension 0
The draws below stay inside these ranges and needn't reach their ends.
There are 2 independent parts, one for each index of `grp`. The reference program is written for one: setup_inputs(seed, part) draws one part's arguments, and reference() takes and returns one part's arrays. A program takes and returns all parts, laid end to end along the dimension named above; an argument that names none is the same for every part. Nothing has to cross between parts.
Inputs may be any that keep to these rules, and one draw needn't show every extreme that they name: doc_ids never fall along the sequence; each document has at most 768 positions.
All inputs are finite; a program needn't handle non-finite values.
Results may differ from the reference program's by a relative error of at most 0.011.
Values may be sent and summed in bfloat16 or wider, within the bound.
A program may use at most 64 MiB of HBM per device.

```python
import math
import jax
import jax.numpy as jnp
import numpy as np
from jax import lax

D = 2048
HEADS = 16
HD = 64
DA = 1024
SEG = 64
LEFT = 8
MAXREL = 256
NREL = 513
LAYERS = 2
TOK_DEV = 256
TOKENS = 1024
DOCS = 2


def draw_rel_bias(key, part):
    base_key = jax.random.fold_in(key, 11)
    table = jnp.clip(jax.random.normal(base_key, (HEADS, NREL), jnp.float32), -4.0, 4.0)
    return table


def block_scale(rng, extent, shards, least, high):
    def one(position, blocks):
        heights = jax.random.uniform(jax.random.fold_in(jax.random.fold_in(rng, 6), position), (blocks,), jnp.float32, least / len(shards), high / len(shards))
        return jnp.repeat(jnp.exp(heights), extent[position] // blocks).reshape((-1,) + (1,) * (len(extent) - position - 1))

    level = one(*shards[0])
    for cut in shards[1:]:
        level = level * one(*cut)
    return level


def profile(amount, total, most, skew):
    weights = [(1 << 20) // math.isqrt(standing ** skew) + 1 for standing in range(2, amount + 1)]
    rest, holding = total - most - (amount - 1), [1] * (amount - 1)
    while rest > 0:
        candidates = [i for i in range(amount - 1) if holding[i] < most]
        whole, left = sum([weights[i] for i in candidates]), rest
        for i in candidates:
            extra = min(most - holding[i], max(1, left * weights[i] // whole), rest)
            holding[i] = holding[i] + extra
            rest = rest - extra
    return np.array([most] + holding)


def uneven_parts(own_key, count, total, bound, lean):
    if count == 2:
        one = jax.random.randint(own_key, (), max(1, total - bound), min(bound, total - 1) + 1)
        return jnp.stack([one, total - one])
    tallies = jnp.asarray(profile(count, total, bound, lean), jnp.int32)
    couples = (count - 1) // 2
    giver, taker = tallies[1:1 + 2 * couples:2], tallies[2:2 + 2 * couples:2]
    slack = jnp.minimum(giver - 1, bound - taker)
    shifted = jax.random.randint(jax.random.fold_in(own_key, 1), (couples,), 0, 1 << 20) % (slack + 1)
    tallies = tallies.at[1:1 + 2 * couples:2].set(giver - shifted).at[2:2 + 2 * couples:2].set(taker + shifted)
    return tallies[jax.random.permutation(jax.random.fold_in(own_key, 2), count)]


def noise(key, shape, scale, most, cuts=(), kind=jnp.bfloat16):
    values = scale * jax.random.normal(key, shape, jnp.float32)
    if cuts:
        values = values * block_scale(key, shape, cuts, -0.22, 0.18)
    return jnp.clip(values, -most, most).astype(kind)


def setup_inputs(seed: int = 0, part: int = 0) -> dict:
    key_of = jax.random.split(jax.random.key(seed), 11)
    part_splits = jax.random.split(jax.random.fold_in(key_of[10], part), 11)
    stream = noise(part_splits[0], (TOKENS, D), 1.0, 6.0, ((0, 4),))
    doc_ids = jnp.searchsorted(jnp.cumsum(uneven_parts(part_splits[1], DOCS, TOKENS, 3 * TOK_DEV, 1)), jnp.arange(TOKENS), side="right").astype(jnp.int32)
    norm_gain = jnp.clip(1.0 + 0.18 * jax.random.normal(key_of[2], (LAYERS, D), jnp.float32), 0.1, 1.9)
    query_weight = noise(key_of[3], (LAYERS, D, DA), D ** -0.5, 0.125, ((1, 4), (2, 4)))
    key_weight = noise(key_of[4], (LAYERS, D, DA), D ** -0.5, 0.125, ((1, 4), (2, 4)))
    value_weight = noise(key_of[5], (LAYERS, D, DA), D ** -0.5, 0.125, ((1, 4), (2, 4)))
    out_weight = noise(key_of[6], (LAYERS, DA, D), (DA // 16) ** -0.5, 0.75, ((1, 4), (2, 4)))
    query_gain = jnp.clip(1.0 + 0.18 * jax.random.normal(key_of[7], (LAYERS, HD), jnp.float32), 0.1, 1.9)
    key_gain = jnp.clip(1.0 + 0.18 * jax.random.normal(key_of[8], (LAYERS, HD), jnp.float32), 0.1, 1.9)
    rel_bias = draw_rel_bias(jax.random.fold_in(key_of[10], 71), part)
    return {"stream": stream, "doc_ids": doc_ids, "norm_gain": norm_gain, "query_weight": query_weight, "key_weight": key_weight, "value_weight": value_weight, "out_weight": out_weight, "query_gain": query_gain, "key_gain": key_gain, "rel_bias": rel_bias}


epsilon = 1e-06

def row_norm(values, gain):
    return values * lax.rsqrt(lax.optimization_barrier(jnp.mean(values * values, axis=-1, keepdims=True)) + epsilon) * gain

def band_of(values, count):
    blocks = values.reshape((count + LEFT, SEG) + values.shape[1:])
    stacked = jnp.stack([blocks[earlier:earlier + count] for earlier in range(LEFT + 1)], axis=1)
    return stacked.reshape((count, (LEFT + 1) * SEG) + values.shape[1:])

def reference(stream, doc_ids, norm_gain, query_weight, key_weight, value_weight, out_weight, query_gain, key_gain, rel_bias):
    total = stream.shape[0]
    count = total // SEG
    reach = LEFT * SEG
    width = (LEFT + 1) * SEG
    scale = HD ** (-0.5)
    distance = reach + jnp.arange(SEG, dtype=jnp.int32)[:, None] - jnp.arange(width, dtype=jnp.int32)[None, :]
    index = (jnp.clip(distance, -MAXREL, MAXREL) + MAXREL).astype(jnp.int32)
    table = jnp.take(rel_bias.astype(jnp.float32), index, axis=1)
    padded_docs = jnp.concatenate([jnp.full((reach,), -1, jnp.int32), doc_ids.astype(jnp.int32)])
    doc_band = band_of(padded_docs, count)
    key_pos = SEG * jnp.arange(count, dtype=jnp.int32)[:, None] - reach + jnp.arange(width, dtype=jnp.int32)[None, :]
    allowed = (key_pos >= 0)[:, None, :] & (doc_band[:, None, :] == doc_ids.reshape(count, SEG)[:, :, None])
    x = stream
    for layer in range(LAYERS):
        widened = x.astype(jnp.float32)
        normed = row_norm(widened, norm_gain[layer]).astype(jnp.bfloat16)
        q_raw = jnp.dot(normed, query_weight[layer], preferred_element_type=jnp.float32).reshape(total, HEADS, HD)
        k_raw = jnp.dot(normed, key_weight[layer], preferred_element_type=jnp.float32).reshape(total, HEADS, HD)
        v_raw = jnp.dot(normed, value_weight[layer], preferred_element_type=jnp.float32).reshape(total, HEADS, HD)
        query = row_norm(q_raw, query_gain[layer]).astype(jnp.bfloat16)
        keys = row_norm(k_raw, key_gain[layer]).astype(jnp.bfloat16)
        values = v_raw.astype(jnp.bfloat16)

        def one_head(operands):
            head_query, head_keys, head_values, head_table = operands
            pad_keys = jnp.concatenate([jnp.zeros((reach, HD), jnp.bfloat16), head_keys], axis=0)
            pad_values = jnp.concatenate([jnp.zeros((reach, HD), jnp.bfloat16), head_values], axis=0)
            key_band = band_of(pad_keys, count).astype(jnp.float32)
            value_band = band_of(pad_values, count).astype(jnp.float32)
            blocks = head_query.reshape(count, SEG, HD).astype(jnp.float32)
            scores = jnp.einsum('nqd,nkd->nqk', blocks, key_band) * scale + head_table[None]
            scores = jnp.where(allowed, scores, -1e+30)
            peak = lax.optimization_barrier(jnp.max(scores, axis=-1, keepdims=True))
            expo = jnp.exp(scores - peak)
            weights = (expo / lax.optimization_barrier(jnp.sum(expo, axis=-1, keepdims=True))).astype(jnp.bfloat16)
            mixed = jnp.einsum('nqk,nkd->nqd', weights.astype(jnp.float32), value_band)
            return mixed.astype(jnp.bfloat16).reshape(total, HD)
        attended = lax.map(one_head, (query.transpose(1, 0, 2), keys.transpose(1, 0, 2), values.transpose(1, 0, 2), table))
        attended = attended.transpose(1, 0, 2).reshape(total, HEADS * HD)
        x = (widened + jnp.dot(attended, out_weight[layer], preferred_element_type=jnp.float32)).astype(jnp.bfloat16)
    return x
```

```python
import functools

import jax
import jax.numpy as jnp
from jax import lax
from jax.experimental import pallas as pl
from jax.experimental.pallas import tpu as pltpu
from jax.sharding import PartitionSpec as P

SEG = 64
LEFT = 8
MAXREL = 256
LAYERS = 2


epsilon = 1e-06


def shifted(value, axis, steps):
    count = lax.axis_size(axis)
    initial, last = (max(0, -steps), min(count, count - steps))
    return lax.ppermute(value, axis, [(source, source + steps) for source in range(initial, last)])


def row_norm(values, gain):
    return values * lax.rsqrt(jnp.mean(values * values, axis=-1, keepdims=True) + epsilon) * gain


def bias_table(rel_bias):
    heads_here = rel_bias.shape[0]
    reach = LEFT * SEG
    width = (LEFT + 1) * SEG
    highest = reach + SEG - 1
    reversed_bias = rel_bias[:, ::-1]
    upper_fill = jnp.broadcast_to(rel_bias[:, -1:], (heads_here, highest - MAXREL))
    flat_row = jnp.concatenate([upper_fill, reversed_bias[:, : MAXREL + SEG]], axis=1)
    lines = [
        flat_row[:, SEG - 1 - position : SEG - 1 - position + width] for position in range(SEG)
    ]
    return jnp.stack(lines, axis=1)


def attend(query, ext_keys, ext_values, ext_docs, own_docs, offset, table):
    rows, heads_here, head_size = query.shape
    count = rows // SEG
    width = (LEFT + 1) * SEG
    blocks = query.reshape(count, SEG, heads_here, head_size)
    key_blocks = ext_keys.reshape(count + LEFT, SEG, heads_here, head_size)
    value_blocks = ext_values.reshape(count + LEFT, SEG, heads_here, head_size)
    doc_blocks = ext_docs.reshape(count + LEFT, SEG)
    score_parts = [
        jnp.einsum(
            "nqhd,nkhd->nhqk",
            blocks,
            key_blocks[earlier : earlier + count],
            preferred_element_type=jnp.float32,
        )
        for earlier in range(LEFT + 1)
    ]
    scores = jnp.concatenate(score_parts, axis=-1)
    scores = scores * head_size ** (-0.5) + table[None]
    doc_band = jnp.concatenate(
        [doc_blocks[earlier : earlier + count] for earlier in range(LEFT + 1)], axis=1
    )
    key_pos = (
        offset
        + SEG * jnp.arange(count, dtype=jnp.int32)[:, None]
        - LEFT * SEG
        + jnp.arange(width, dtype=jnp.int32)[None, :]
    )
    allowed = (key_pos >= 0)[:, None, None, :] & (
        doc_band[:, None, None, :] == own_docs.reshape(count, SEG)[:, None, :, None]
    )
    scores = jnp.where(allowed, scores, -1e30)
    peak = jnp.max(scores, axis=-1, keepdims=True)
    expo = jnp.exp(scores - peak)
    weights = (expo / jnp.sum(expo, axis=-1, keepdims=True)).astype(jnp.bfloat16)
    mixed = jnp.zeros((count, SEG, heads_here, head_size), jnp.float32)
    for earlier in range(LEFT + 1):
        part_weights = weights[..., earlier * SEG : (earlier + 1) * SEG]
        mixed = mixed + jnp.einsum(
            "nhqk,nkhd->nqhd",
            part_weights,
            value_blocks[earlier : earlier + count],
            preferred_element_type=jnp.float32,
        )
    return mixed.astype(jnp.bfloat16).reshape(rows, heads_here * head_size)


def on_device(
    stream,
    doc_ids,
    norm_gain,
    query_weight,
    key_weight,
    value_weight,
    out_weight,
    query_gain,
    key_gain,
    rel_bias,
):
    rows = stream.shape[0]
    heads_here = rel_bias.shape[0]
    head_size = query_gain.shape[1]
    local_width = heads_here * head_size
    reach = LEFT * SEG
    depth = -(-reach // rows)
    offset = lax.axis_index("sp") * rows
    col_width = out_weight.shape[2]
    col_start = lax.axis_index("tp") * col_width
    table = bias_table(rel_bias)
    x = stream
    for layer in range(LAYERS):
        widened = x.astype(jnp.float32)
        normed = row_norm(widened, norm_gain[layer]).astype(jnp.bfloat16)
        own_cols = normed
        q_raw = jnp.dot(
            own_cols,
            lax.all_gather(query_weight[layer], "sp", axis=0, tiled=True),
            preferred_element_type=jnp.float32,
        )
        k_raw = jnp.dot(
            normed,
            lax.all_gather(key_weight[layer], "sp", axis=0, tiled=True),
            preferred_element_type=jnp.float32,
        )
        v_raw = jnp.dot(
            normed,
            lax.all_gather(value_weight[layer], "sp", axis=0, tiled=True),
            preferred_element_type=jnp.float32,
        )
        query = row_norm(q_raw.reshape(rows, heads_here, head_size), query_gain[layer]).astype(
            jnp.bfloat16
        )
        keys = row_norm(
            k_raw.reshape(normed.shape[0], heads_here, head_size), key_gain[layer]
        ).astype(jnp.bfloat16)
        values = v_raw.astype(jnp.bfloat16)
        flat_keys = keys.reshape(rows, local_width)
        tail = (flat_keys, values, doc_ids)
        received = [
            shifted((tail[0], tail[1], tail[2]), "sp", distance_back)
            for distance_back in range(depth, 0, -1)
        ]
        ext_keys = jnp.concatenate([item[0] for item in received] + [flat_keys], axis=0)
        ext_values = jnp.concatenate([item[1] for item in received] + [values], axis=0)
        ext_docs = jnp.concatenate([item[2] for item in received] + [doc_ids], axis=0)
        ext_keys = ext_keys.reshape(reach + rows, heads_here, head_size)
        ext_values = ext_values.reshape(reach + rows, heads_here, head_size)
        attended = attend(query, ext_keys, ext_values, ext_docs, doc_ids, offset, table)
        all_heads = lax.all_gather(attended, "tp", axis=1, tiled=True)
        projected = jnp.dot(
            all_heads,
            lax.all_gather(out_weight[layer], "sp", axis=0, tiled=True),
            preferred_element_type=jnp.float32,
        )
        own_cols = lax.dynamic_slice_in_dim(widened, col_start, col_width, 1)
        new_cols = (own_cols + projected).astype(jnp.bfloat16)
        x = lax.all_gather(new_cols, "tp", axis=1, tiled=True)
    return x


MESH = pl.DeviceIdType.MESH
NEG = -1e30


def fused_kernel(
    sizes,
    x_ref,
    docs_ref,
    ngain_ref,
    wt_ref,
    woin_ref,
    qgain_ref,
    kgain_ref,
    frow_ref,
    out_ref,
    xg,
    wq,
    wo,
    docs,
    dcol,
    ag,
    fin,
    bias,
    nb,
    q_s,
    k_s,
    v_s,
    o_s,
    doc_send,
    doc_recv,
    xz_send,
    xz_recv,
    xa_send,
    xa_recv,
    xb_send,
    xb_recv,
    xc_send,
    xc_recv,
    wz_send,
    wz_recv,
    wy_send,
    wy_recv,
    oz_send,
    oz_recv,
    oy_send,
    oy_recv,
    az_send,
    az_recv,
    at_send,
    at_recv,
    fn_send,
    fn_recv,
):
    groups, seqs, tps = sizes
    rows, width = x_ref.shape
    cols = width // tps
    head = qgain_ref.shape[1]
    layers = wt_ref.shape[0]
    depth = bias.shape[0] - 1
    grp = lax.axis_index("grp")
    s = lax.axis_index("sp")
    t = lax.axis_index("tp")
    other_grp = 1 - grp
    core = t + 1 - 2 * lax.rem(t, 2)
    side = lax.rem(t + 2, tps)
    diag = core + 2 - 4 * (core // 2)
    started = []

    def send(src, dst, send_sem, recv_sem, where):
        copy = pltpu.make_async_remote_copy(
            src_ref=src,
            dst_ref=dst,
            send_sem=send_sem,
            recv_sem=recv_sem,
            device_id=where,
            device_id_type=MESH,
        )
        copy.start()
        started.append(copy)
        return copy

    def ahead(o):
        return lax.rem(s + o, seqs)

    def behind(o):
        return lax.rem(s + seqs - o, seqs)

    def block_rows(i):
        return pl.ds(pl.multiple_of(i * rows, rows), rows)

    barrier = pltpu.get_barrier_semaphore()
    partners = [{"sp": ahead(o)} for o in range(1, seqs)]
    partners += [{"tp": core}, {"tp": side}, {"grp": other_grp}]
    for where in partners:
        pl.semaphore_signal(barrier, inc=1, device_id=where, device_id_type=MESH)
    pl.semaphore_wait(barrier, len(partners))

    own_cols = pl.ds(pl.multiple_of(t * cols, cols), cols)
    whalf = wt_ref.shape[2] // 2
    ohalf = woin_ref.shape[1] // 2
    wpart = pl.ds(pl.multiple_of(grp * whalf, whalf), whalf)
    opart = pl.ds(pl.multiple_of(grp * ohalf, ohalf), ohalf)
    hops = list(range(1, seqs))

    doc_c = [
        send(docs_ref, docs.at[s], doc_send.at[o], doc_recv.at[o], {"sp": ahead(o)}) for o in hops
    ]
    xz = {
        o: send(
            x_ref.at[:, own_cols],
            xg.at[0, t, block_rows(s), :],
            xz_send.at[0, o],
            xz_recv.at[0, o],
            {"sp": ahead(o)},
        )
        for o in hops
    }

    def send_qkv(layer):
        return {
            o: send(
                wt_ref.at[layer, ahead(o), wpart, :],
                wq.at[layer, s, wpart, :],
                wz_send.at[layer, o],
                wz_recv.at[layer, o],
                {"sp": ahead(o)},
            )
            for o in hops
        }

    def send_out(layer):
        return {
            o: send(
                woin_ref.at[layer, opart, :],
                wo.at[layer, s, opart, :],
                oz_send.at[layer, o],
                oz_recv.at[layer, o],
                {"sp": ahead(o)},
            )
            for o in hops
        }

    def relay_qkv(layer, flying):
        result = []
        for o in hops:
            flying[o].wait_recv()
            block = wq.at[layer, behind(o), wpart, :]
            result.append(
                send(block, block, wy_send.at[layer, o], wy_recv.at[layer, o], {"grp": other_grp})
            )
        return result

    def relay_out(layer, flying):
        result = []
        for o in hops:
            flying[o].wait_recv()
            block = wo.at[layer, behind(o), opart, :]
            result.append(
                send(block, block, oy_send.at[layer, o], oy_recv.at[layer, o], {"grp": other_grp})
            )
        return result

    qkv_fly = send_qkv(0)

    for part in range(tps):
        xg[0, part, block_rows(s), :] = x_ref[:, part * cols : (part + 1) * cols]
    for layer in range(layers):
        wq[layer, s] = wt_ref[layer, s]
        wo[layer, s] = woin_ref[layer]
    docs[s] = docs_ref[...]
    key_seg = lax.broadcasted_iota(jnp.int32, (rows, rows), 0) // SEG
    query_seg = lax.broadcasted_iota(jnp.int32, (rows, rows), 1) // SEG
    for d in range(depth + 1):
        spread = jnp.broadcast_to(frow_ref[d : d + 1, :], (rows, 2 * rows))
        rolled = pltpu.roll(spread, 0, 1, stride=1, stride_axis=0)
        gap = query_seg + (d * rows) // SEG - key_seg
        bias[d] = jnp.where((gap >= 0) & (gap <= LEFT), rolled[:, rows:], NEG)
    for copy in doc_c:
        copy.wait_recv()
    for i in range(seqs):
        dcol[i] = jnp.transpose(jnp.broadcast_to(docs[i, 0:1, :], (128, rows)))

    def spread_tp(layer, first):
        to_core, to_side, to_diag = {}, {}, {}

        def fan(o):
            if o > 0:
                xz[o].wait_recv()
            block = xg.at[layer, t, block_rows(behind(o)), :]
            to_side[o] = send(
                block, block, xb_send.at[layer, o], xb_recv.at[layer, o], {"tp": side}
            )
            to_core[o] = send(
                block, block, xa_send.at[layer, o], xa_recv.at[layer, o], {"tp": core}
            )

        def pass_on(o):
            to_side[o].wait_recv()
            block = xg.at[layer, side, block_rows(behind(o)), :]
            to_diag[o] = send(
                block, block, xc_send.at[layer, o], xc_recv.at[layer, o], {"tp": core}
            )

        order = list(range(first, seqs))
        for place, o in enumerate(order):
            fan(o)
            if place >= 1:
                pass_on(order[place - 1])
        pass_on(order[-1])
        return to_core, to_diag

    def project(layer, o):
        i = behind(o)
        total = jnp.zeros((rows, 1), jnp.float32)
        for part in range(tps):
            piece = xg[layer, part, block_rows(i), :].astype(jnp.float32)
            total = total + jnp.sum(piece * piece, axis=1, keepdims=True)
        factor = lax.rsqrt(total * (1.0 / width) + epsilon)
        for part in range(tps):
            piece = xg[layer, part, block_rows(i), :].astype(jnp.float32)
            gain = ngain_ref[layer : layer + 1, part * cols : (part + 1) * cols]
            nb[:, part * cols : (part + 1) * cols] = (piece * factor * gain).astype(jnp.bfloat16)
        span = width // seqs
        raw = jnp.zeros((3 * head, rows), jnp.float32)
        for part in range(seqs):
            raw = raw + lax.dot_general(
                wq[layer, part],
                nb[:, part * span : (part + 1) * span],
                (((1,), (1,)), ((), ())),
                preferred_element_type=jnp.float32,
            )

        def normal(value, gain):
            mean = jnp.mean(value * value, axis=0, keepdims=True)
            return value * lax.rsqrt(mean + epsilon) * gain

        q_s[i] = (normal(raw[:head], qgain_ref[layer]) * head ** (-0.5)).astype(jnp.bfloat16)
        k_s[i] = jnp.transpose(normal(raw[head : 2 * head], kgain_ref[layer])).astype(jnp.bfloat16)
        v_s[i] = raw[2 * head :].astype(jnp.bfloat16)

    def attention():
        for j in range(seqs):
            pieces = []
            for i in range(max(0, j - depth), j + 1):
                score = jnp.dot(k_s[i], q_s[j], preferred_element_type=jnp.float32)
                same = dcol[i][:, 0:1] == docs[j, 0:1, :]
                pieces.append((i, jnp.where(same, score + bias[j - i], NEG)))
            peak = pieces[0][1].max(axis=0, keepdims=True)
            for _, piece in pieces[1:]:
                peak = jnp.maximum(peak, piece.max(axis=0, keepdims=True))
            mass = jnp.zeros((1, rows), jnp.float32)
            mixed = jnp.zeros((head, rows), jnp.float32)
            for i, piece in pieces:
                expo = jnp.exp(piece - peak)
                mass = mass + jnp.sum(expo, axis=0, keepdims=True)
                mixed = mixed + jnp.dot(
                    v_s[i], expo.astype(jnp.bfloat16), preferred_element_type=jnp.float32
                )
            o_s[lax.rem(j, seqs)] = (mixed / mass).astype(jnp.bfloat16)

    for layer in range(layers):
        last = layer == layers - 1
        first = 1 if layer == 0 else 0
        to_core, to_diag = spread_tp(layer, first)
        if layer == 0:
            project_ready = relay_qkv(0, qkv_fly)
            out_fly = send_out(0)
        for copy in project_ready:
            copy.wait_recv()
        if layer == 0:
            project(layer, 0)
        for o in range(first, seqs):
            to_core[o].wait_recv()
            to_diag[o].wait_recv()
            project(layer, o)
        if layer > 0:
            for copy in outgoing:
                copy.wait_send()
            started[:] = [copy for copy in started if all(copy is not old for old in outgoing)]
        attention()
        outgoing = [
            send(
                o_s.at[ahead(o)],
                ag.at[layer, t, s],
                az_send.at[layer, o],
                az_recv.at[layer, o],
                {"sp": ahead(o)},
            )
            for o in hops
        ]
        if not last:
            qkv_fly = send_qkv(layer + 1)
        ag[layer, t, s] = o_s[s]
        out_ready = relay_out(layer, out_fly)
        for copy in outgoing:
            copy.wait_recv()
        block = ag.at[layer, t]
        across = send(block, block, at_send.at[layer, 0], at_recv.at[layer, 0], {"tp": side})
        beside = send(block, block, at_send.at[layer, 1], at_recv.at[layer, 1], {"tp": core})
        across.wait_recv()
        block = ag.at[layer, side]
        corner = send(block, block, at_send.at[layer, 2], at_recv.at[layer, 2], {"tp": core})
        for copy in out_ready:
            copy.wait_recv()
        beside.wait_recv()
        corner.wait_recv()
        heads_all = ag[layer].reshape(tps * seqs * head, rows)
        weight = wo[layer].reshape(-1, cols)
        product = lax.dot_general(
            heads_all,
            weight,
            (((0,), (0,)), ((), ())),
            preferred_element_type=jnp.float32,
        )
        kept = xg[layer, t, block_rows(s), :].astype(jnp.float32)
        fresh = (kept + product).astype(jnp.bfloat16)
        if not last:
            xg[layer + 1, t, block_rows(s), :] = fresh
            mine = xg.at[layer + 1, t, block_rows(s), :]
            xz = {
                o: send(
                    mine,
                    mine,
                    xz_send.at[layer + 1, o],
                    xz_recv.at[layer + 1, o],
                    {"sp": ahead(o)},
                )
                for o in hops
            }
            project_ready = relay_qkv(layer + 1, qkv_fly)
            out_fly = send_out(layer + 1)
        else:
            fin[t] = fresh
            cuts = fn_send.shape[0]
            tall = rows // cuts
            crossing, beside = [], []
            for c in range(cuts):
                part = fin.at[t, pl.ds(c * tall, tall), :]
                crossing.append(send(part, part, fn_send.at[c, 0], fn_recv.at[c, 0], {"tp": side}))
                beside.append(send(part, part, fn_send.at[c, 1], fn_recv.at[c, 1], {"tp": core}))
            for c in range(cuts):
                crossing[c].wait_recv()
                part = fin.at[side, pl.ds(c * tall, tall), :]
                beside.append(send(part, part, fn_send.at[c, 2], fn_recv.at[c, 2], {"tp": core}))
            for copy in beside:
                copy.wait_recv()
            for part in range(tps):
                out_ref[:, part * cols : (part + 1) * cols] = fin[part]
    for copy in started:
        copy.wait_send()


def fused_device(
    sizes,
    stream,
    doc_ids,
    norm_gain,
    query_weight,
    key_weight,
    value_weight,
    out_weight,
    query_gain,
    key_gain,
    rel_bias,
):
    groups, seqs, tps = sizes
    rows, width = stream.shape
    cols = width // tps
    layers, deep, _ = query_weight.shape
    head = query_gain.shape[1]
    depth = -(-LEFT * SEG // rows)

    def turned(weight):
        return weight.reshape(layers, deep, seqs, head).transpose(0, 2, 3, 1)

    wt = jnp.concatenate(
        [turned(query_weight), turned(key_weight), turned(value_weight)], axis=2
    )
    row = lax.dynamic_index_in_dim(rel_bias, lax.axis_index("sp"), 0, keepdims=False)
    span = (depth + 2) * rows
    line = jnp.concatenate([row, jnp.broadcast_to(row[-1:], (span - row.shape[0],))])
    frow = jnp.stack([line[d * rows : (d + 2) * rows] for d in range(depth + 1)])
    docs8 = jnp.broadcast_to(doc_ids.astype(jnp.float32)[None], (8, rows))
    dma = pltpu.SemaphoreType.DMA
    bf16 = jnp.bfloat16
    scratch = [
        pltpu.VMEM((layers, tps, seqs * rows, cols), bf16),
        pltpu.VMEM((layers, seqs, 3 * head, deep), bf16),
        pltpu.VMEM((layers, seqs) + out_weight.shape[1:], bf16),
        pltpu.VMEM((seqs, 8, rows), jnp.float32),
        pltpu.VMEM((seqs, rows, 128), jnp.float32),
        pltpu.VMEM((layers, tps, seqs, head, rows), bf16),
        pltpu.VMEM((tps, rows, cols), bf16),
        pltpu.VMEM((depth + 1, rows, rows), jnp.float32),
        pltpu.VMEM((rows, width), bf16),
        pltpu.VMEM((seqs, head, rows), bf16),
        pltpu.VMEM((seqs, rows, head), bf16),
        pltpu.VMEM((seqs, head, rows), bf16),
        pltpu.VMEM((seqs, head, rows), bf16),
    ]
    scratch += [dma((seqs,))] * 2 + [dma((layers, seqs))] * 16
    scratch += [dma((layers, seqs))] * 2 + [dma((layers, 3))] * 2 + [dma((2, 3))] * 2
    return pl.pallas_call(
        functools.partial(fused_kernel, sizes),
        name="fused_layers",
        out_shape=jax.ShapeDtypeStruct((rows, width), bf16),
        in_specs=[pl.BlockSpec(memory_space=pltpu.VMEM)] * 8,
        out_specs=pl.BlockSpec(memory_space=pltpu.VMEM),
        scratch_shapes=scratch,
        compiler_params=pltpu.CompilerParams(
            collective_id=0, has_side_effects=True, vmem_limit_bytes=60 * 1024 * 1024
        ),
    )(
        stream,
        docs8,
        norm_gain,
        wt,
        out_weight,
        query_gain[..., None],
        key_gain[..., None],
        frow,
    )


def solution(mesh):
    placed = (
        P(("grp", "sp"), None),
        P(("grp", "sp")),
        P(),
        P(None, "sp", "tp"),
        P(None, "sp", "tp"),
        P(None, "sp", "tp"),
        P(None, "sp", "tp"),
        P(),
        P(),
        P("tp", None),
    )
    sizes = tuple(mesh.shape[axis] for axis in ("grp", "sp", "tp"))

    def body(*args):
        one_head_each = args[-1].shape[0] == sizes[1]
        fits = sizes[0] == 2 and sizes[2] == 4 and args[0].shape[0] == MAXREL
        if one_head_each and fits:
            return fused_device(sizes, *args)
        return on_device(*args)

    return jax.shard_map(
        body, mesh=mesh, in_specs=placed, out_specs=P(("grp", "sp"), None), check_vma=False
    )
```

```python
import functools

import jax
import jax.numpy as jnp
from jax import lax
from jax.experimental import pallas as pl
from jax.experimental.pallas import tpu as pltpu
from jax.sharding import PartitionSpec as P

SEG = 64
LEFT = 8
MAXREL = 256
LAYERS = 2


epsilon = 1e-06


def shifted(value, axis, steps):
    count = lax.axis_size(axis)
    initial, last = (max(0, -steps), min(count, count - steps))
    return lax.ppermute(value, axis, [(source, source + steps) for source in range(initial, last)])


def row_norm(values, gain):
    return values * lax.rsqrt(jnp.mean(values * values, axis=-1, keepdims=True) + epsilon) * gain


def bias_table(rel_bias):
    heads_here = rel_bias.shape[0]
    reach = LEFT * SEG
    width = (LEFT + 1) * SEG
    highest = reach + SEG - 1
    reversed_bias = rel_bias[:, ::-1]
    upper_fill = jnp.broadcast_to(rel_bias[:, -1:], (heads_here, highest - MAXREL))
    flat_row = jnp.concatenate([upper_fill, reversed_bias[:, : MAXREL + SEG]], axis=1)
    lines = [
        flat_row[:, SEG - 1 - position : SEG - 1 - position + width] for position in range(SEG)
    ]
    return jnp.stack(lines, axis=1)


def attend(query, ext_keys, ext_values, ext_docs, own_docs, offset, table):
    rows, heads_here, head_size = query.shape
    count = rows // SEG
    width = (LEFT + 1) * SEG
    blocks = query.reshape(count, SEG, heads_here, head_size)
    key_blocks = ext_keys.reshape(count + LEFT, SEG, heads_here, head_size)
    value_blocks = ext_values.reshape(count + LEFT, SEG, heads_here, head_size)
    doc_blocks = ext_docs.reshape(count + LEFT, SEG)
    score_parts = [
        jnp.einsum(
            "nqhd,nkhd->nhqk",
            blocks,
            key_blocks[earlier : earlier + count],
            preferred_element_type=jnp.float32,
        )
        for earlier in range(LEFT + 1)
    ]
    scores = jnp.concatenate(score_parts, axis=-1)
    scores = scores * head_size ** (-0.5) + table[None]
    doc_band = jnp.concatenate(
        [doc_blocks[earlier : earlier + count] for earlier in range(LEFT + 1)], axis=1
    )
    key_pos = (
        offset
        + SEG * jnp.arange(count, dtype=jnp.int32)[:, None]
        - LEFT * SEG
        + jnp.arange(width, dtype=jnp.int32)[None, :]
    )
    allowed = (key_pos >= 0)[:, None, None, :] & (
        doc_band[:, None, None, :] == own_docs.reshape(count, SEG)[:, None, :, None]
    )
    scores = jnp.where(allowed, scores, -1e30)
    peak = jnp.max(scores, axis=-1, keepdims=True)
    expo = jnp.exp(scores - peak)
    weights = (expo / jnp.sum(expo, axis=-1, keepdims=True)).astype(jnp.bfloat16)
    mixed = jnp.zeros((count, SEG, heads_here, head_size), jnp.float32)
    for earlier in range(LEFT + 1):
        part_weights = weights[..., earlier * SEG : (earlier + 1) * SEG]
        mixed = mixed + jnp.einsum(
            "nhqk,nkhd->nqhd",
            part_weights,
            value_blocks[earlier : earlier + count],
            preferred_element_type=jnp.float32,
        )
    return mixed.astype(jnp.bfloat16).reshape(rows, heads_here * head_size)


def on_device(
    stream,
    doc_ids,
    norm_gain,
    query_weight,
    key_weight,
    value_weight,
    out_weight,
    query_gain,
    key_gain,
    rel_bias,
):
    rows = stream.shape[0]
    heads_here = rel_bias.shape[0]
    head_size = query_gain.shape[1]
    local_width = heads_here * head_size
    reach = LEFT * SEG
    depth = -(-reach // rows)
    offset = lax.axis_index("sp") * rows
    col_width = out_weight.shape[2]
    col_start = lax.axis_index("tp") * col_width
    table = bias_table(rel_bias)
    x = stream
    for layer in range(LAYERS):
        widened = x.astype(jnp.float32)
        normed = row_norm(widened, norm_gain[layer]).astype(jnp.bfloat16)
        own_cols = normed
        q_raw = jnp.dot(
            own_cols,
            lax.all_gather(query_weight[layer], "sp", axis=0, tiled=True),
            preferred_element_type=jnp.float32,
        )
        k_raw = jnp.dot(
            normed,
            lax.all_gather(key_weight[layer], "sp", axis=0, tiled=True),
            preferred_element_type=jnp.float32,
        )
        v_raw = jnp.dot(
            normed,
            lax.all_gather(value_weight[layer], "sp", axis=0, tiled=True),
            preferred_element_type=jnp.float32,
        )
        query = row_norm(q_raw.reshape(rows, heads_here, head_size), query_gain[layer]).astype(
            jnp.bfloat16
        )
        keys = row_norm(
            k_raw.reshape(normed.shape[0], heads_here, head_size), key_gain[layer]
        ).astype(jnp.bfloat16)
        values = v_raw.astype(jnp.bfloat16)
        flat_keys = keys.reshape(rows, local_width)
        tail = (flat_keys, values, doc_ids)
        received = [
            shifted((tail[0], tail[1], tail[2]), "sp", distance_back)
            for distance_back in range(depth, 0, -1)
        ]
        ext_keys = jnp.concatenate([item[0] for item in received] + [flat_keys], axis=0)
        ext_values = jnp.concatenate([item[1] for item in received] + [values], axis=0)
        ext_docs = jnp.concatenate([item[2] for item in received] + [doc_ids], axis=0)
        ext_keys = ext_keys.reshape(reach + rows, heads_here, head_size)
        ext_values = ext_values.reshape(reach + rows, heads_here, head_size)
        attended = attend(query, ext_keys, ext_values, ext_docs, doc_ids, offset, table)
        all_heads = lax.all_gather(attended, "tp", axis=1, tiled=True)
        projected = jnp.dot(
            all_heads,
            lax.all_gather(out_weight[layer], "sp", axis=0, tiled=True),
            preferred_element_type=jnp.float32,
        )
        own_cols = lax.dynamic_slice_in_dim(widened, col_start, col_width, 1)
        new_cols = (own_cols + projected).astype(jnp.bfloat16)
        x = lax.all_gather(new_cols, "tp", axis=1, tiled=True)
    return x


MESH = pl.DeviceIdType.MESH
NEG = -1e30


def fused_kernel(
    sizes,
    x_ref,
    docs_ref,
    ngain_ref,
    qw_ref,
    kw_ref,
    vw_ref,
    woin_ref,
    qgain_ref,
    kgain_ref,
    bias_ref,
    out_ref,
    wt_ref,
    xg,
    wq,
    wo,
    docs,
    dcol,
    ag,
    fin,
    bias,
    nb,
    q_s,
    k_s,
    v_s,
    o_s,
    doc_send,
    doc_recv,
    xz_send,
    xz_recv,
    xa_send,
    xa_recv,
    xb_send,
    xb_recv,
    xc_send,
    xc_recv,
    wz_send,
    wz_recv,
    wy_send,
    wy_recv,
    oz_send,
    oz_recv,
    oy_send,
    oy_recv,
    az_send,
    az_recv,
    at_send,
    at_recv,
    fn_send,
    fn_recv,
):
    groups, seqs, tps = sizes
    rows, width = x_ref.shape
    cols = width // tps
    head = qgain_ref.shape[1]
    layers = wt_ref.shape[0]
    depth = bias.shape[0] - 1
    grp = lax.axis_index("grp")
    s = lax.axis_index("sp")
    t = lax.axis_index("tp")
    other_grp = 1 - grp
    core = t + 1 - 2 * lax.rem(t, 2)
    side = lax.rem(t + 2, tps)
    diag = core + 2 - 4 * (core // 2)
    started = []

    def send(src, dst, send_sem, recv_sem, where):
        copy = pltpu.make_async_remote_copy(
            src_ref=src,
            dst_ref=dst,
            send_sem=send_sem,
            recv_sem=recv_sem,
            device_id=where,
            device_id_type=MESH,
        )
        copy.start()
        started.append(copy)
        return copy

    def ahead(o):
        return lax.rem(s + o, seqs)

    def behind(o):
        return lax.rem(s + seqs - o, seqs)

    def block_rows(i):
        return pl.ds(pl.multiple_of(i * rows, rows), rows)

    barrier = pltpu.get_barrier_semaphore()
    partners = [{"sp": ahead(o)} for o in range(1, seqs)]
    partners += [{"tp": core}, {"tp": side}, {"grp": other_grp}]
    for where in partners:
        pl.semaphore_signal(barrier, inc=1, device_id=where, device_id_type=MESH)
    pl.semaphore_wait(barrier, len(partners))

    own_cols = pl.ds(pl.multiple_of(t * cols, cols), cols)
    whalf = wt_ref.shape[2] // 2
    ohalf = woin_ref.shape[1] // 2
    wpart = pl.ds(pl.multiple_of(grp * whalf, whalf), whalf)
    opart = pl.ds(pl.multiple_of(grp * ohalf, ohalf), ohalf)
    hops = list(range(1, seqs))

    doc_c = [
        send(docs_ref, docs.at[s], doc_send.at[o], doc_recv.at[o], {"sp": ahead(o)}) for o in hops
    ]
    def passing(layer, way, k, arriving):
        block = s - k if way == 0 else s + k
        if arriving:
            block = block - 1 if way == 0 else block + 1
        inside = block >= 0 if way == 0 else block < seqs
        return block, inside

    def onward(layer, way, k):
        block, inside = passing(layer, way, k, False)
        open_end = s < seqs - 1 if way == 0 else s > 0
        place = xg.at[layer, t, block_rows(block), :]
        copy = pltpu.make_async_remote_copy(
            src_ref=x_ref.at[:, own_cols] if layer == 0 and k == 0 else place,
            dst_ref=place,
            send_sem=xz_send.at[layer, way, k],
            recv_sem=xz_recv.at[layer, way, k],
            device_id={"sp": s + 1 if way == 0 else s - 1},
            device_id_type=MESH,
        )
        return copy, inside & open_end

    def start_onward(layer, way, k):
        copy, valid = onward(layer, way, k)

        @pl.when(valid)
        def _():
            copy.start()

    def tp_copy(layer, kind, block):
        held = side if kind == 2 else t
        place = xg.at[layer, held, block_rows(block), :]
        send_sem, recv_sem = ((xa_send, xa_recv), (xb_send, xb_recv), (xc_send, xc_recv))[kind]
        return pltpu.make_async_remote_copy(
            src_ref=place,
            dst_ref=place,
            send_sem=send_sem.at[layer, block],
            recv_sem=recv_sem.at[layer, block],
            device_id={"tp": side if kind == 1 else core},
            device_id_type=MESH,
        )

    for way in (0, 1):
        start_onward(0, way, 0)

    def send_qkv(layer):
        return {
            o: send(
                wt_ref.at[layer, ahead(o), wpart, :],
                wq.at[layer, s, wpart, :],
                wz_send.at[layer, o],
                wz_recv.at[layer, o],
                {"sp": ahead(o)},
            )
            for o in hops
        }

    def send_out(layer):
        return {
            o: send(
                woin_ref.at[layer, opart, :],
                wo.at[layer, s, opart, :],
                oz_send.at[layer, o],
                oz_recv.at[layer, o],
                {"sp": ahead(o)},
            )
            for o in hops
        }

    def relay_qkv(layer, flying):
        result = []
        for o in hops:
            flying[o].wait_recv()
            block = wq.at[layer, behind(o), wpart, :]
            result.append(
                send(block, block, wy_send.at[layer, o], wy_recv.at[layer, o], {"grp": other_grp})
            )
        return result

    def relay_out(layer, flying):
        result = []
        for o in hops:
            flying[o].wait_recv()
            block = wo.at[layer, behind(o), opart, :]
            result.append(
                send(block, block, oy_send.at[layer, o], oy_recv.at[layer, o], {"grp": other_grp})
            )
        return result

    for part in range(tps):
        xg[0, part, block_rows(s), :] = x_ref[:, part * cols : (part + 1) * cols]
    for layer in range(layers):
        for which, source in enumerate((qw_ref, kw_ref, vw_ref)):
            turned = jnp.transpose(source[layer])
            for i in range(seqs):
                wt_ref[layer, i, which * head : (which + 1) * head, :] = turned[
                    i * head : (i + 1) * head, :
                ]
        wo[layer, s] = woin_ref[layer]
        wq[layer, s] = wt_ref[layer, s]
    docs[s] = docs_ref[...]
    qkv_fly = send_qkv(0)
    key_seg = lax.broadcasted_iota(jnp.int32, (rows, rows), 0) // SEG
    query_seg = lax.broadcasted_iota(jnp.int32, (rows, rows), 1) // SEG
    for d in range(depth + 1):
        spread = jnp.broadcast_to(
            bias_ref[pl.ds(s, 1), d * rows : (d + 2) * rows], (rows, 2 * rows)
        )
        rolled = pltpu.roll(spread, 0, 1, stride=1, stride_axis=0)
        gap = query_seg + (d * rows) // SEG - key_seg
        bias[d] = jnp.where((gap >= 0) & (gap <= LEFT), rolled[:, rows:], NEG)
    for copy in doc_c:
        copy.wait_recv()
    for i in range(seqs):
        dcol[i] = jnp.transpose(jnp.broadcast_to(docs[i, 0:1, :], (128, rows)))

    def fan(layer, block):
        tp_copy(layer, 1, block).start()
        tp_copy(layer, 0, block).start()

    def pass_on(layer, block):
        tp_copy(layer, 1, block).wait_recv()
        tp_copy(layer, 2, block).start()

    def spread_tp(layer, own_too):
        if own_too:
            fan(layer, s)
        for k in range(seqs - 1):
            for way in (0, 1):
                block, inside = passing(layer, way, k, True)

                @pl.when(inside)
                def _(block=block, way=way, k=k):
                    onward(layer, way, k)[0].wait_recv()
                    if k + 1 < seqs - 1:
                        start_onward(layer, way, k + 1)
                    fan(layer, block)

            if k == 0 and own_too:
                pass_on(layer, s)
            pass_slots(layer, k - 1)
        pass_slots(layer, seqs - 2)

    def pass_slots(layer, k):
        if k < 0:
            return
        for way in (0, 1):
            block, inside = passing(layer, way, k, True)

            @pl.when(inside)
            def _(block=block):
                pass_on(layer, block)

    def nth(v):
        orders = [
            sorted((b for b in range(seqs) if b != c), key=lambda b: abs(b - c))
            for c in range(seqs)
        ]
        block = orders[0][v - 1]
        for c in range(1, seqs):
            block = jnp.where(s == c, orders[c][v - 1], block)
        return block

    def project(layer, i):
        total = jnp.zeros((rows, 1), jnp.float32)
        for part in range(tps):
            piece = xg[layer, part, block_rows(i), :].astype(jnp.float32)
            total = total + jnp.sum(piece * piece, axis=1, keepdims=True)
        factor = lax.rsqrt(total * (1.0 / width) + epsilon)
        for part in range(tps):
            piece = xg[layer, part, block_rows(i), :].astype(jnp.float32)
            gain = ngain_ref[layer : layer + 1, part * cols : (part + 1) * cols]
            nb[:, part * cols : (part + 1) * cols] = (piece * factor * gain).astype(jnp.bfloat16)
        span = width // seqs
        raw = jnp.zeros((3 * head, rows), jnp.float32)
        for part in range(seqs):
            raw = raw + lax.dot_general(
                wq[layer, part],
                nb[:, part * span : (part + 1) * span],
                (((1,), (1,)), ((), ())),
                preferred_element_type=jnp.float32,
            )

        def normal(value, gain):
            mean = jnp.mean(value * value, axis=0, keepdims=True)
            column = jnp.transpose(jnp.broadcast_to(gain, (128, head)))[:, 0:1]
            return value * lax.rsqrt(mean + epsilon) * column

        q_s[i] = (normal(raw[:head], qgain_ref[layer : layer + 1, :]) * head ** (-0.5)).astype(jnp.bfloat16)
        k_s[i] = jnp.transpose(normal(raw[head : 2 * head], kgain_ref[layer : layer + 1, :])).astype(jnp.bfloat16)
        v_s[i] = raw[2 * head :].astype(jnp.bfloat16)

    def attention():
        for j in range(seqs):
            pieces = []
            for i in range(max(0, j - depth), j + 1):
                score = jnp.dot(k_s[i], q_s[j], preferred_element_type=jnp.float32)
                same = dcol[i][:, 0:1] == docs[j, 0:1, :]
                pieces.append((i, jnp.where(same, score + bias[j - i], NEG)))
            peak = pieces[0][1].max(axis=0, keepdims=True)
            for _, piece in pieces[1:]:
                peak = jnp.maximum(peak, piece.max(axis=0, keepdims=True))
            mass = jnp.zeros((1, rows), jnp.float32)
            mixed = jnp.zeros((head, rows), jnp.float32)
            for i, piece in pieces:
                expo = jnp.exp(piece - peak)
                mass = mass + jnp.sum(expo, axis=0, keepdims=True)
                mixed = mixed + jnp.dot(
                    v_s[i], expo.astype(jnp.bfloat16), preferred_element_type=jnp.float32
                )
            o_s[lax.rem(j, seqs)] = (mixed / mass).astype(jnp.bfloat16)

    for layer in range(layers):
        last = layer == layers - 1
        spread_tp(layer, layer > 0)
        if layer == 0:
            project_ready = relay_qkv(0, qkv_fly)
            out_fly = send_out(0)
        for copy in project_ready:
            copy.wait_recv()
        for v in range(seqs):
            block = nth(v) if v else s
            if v or layer > 0:
                tp_copy(layer, 0, block).wait_recv()
                tp_copy(layer, 2, block).wait_recv()
            project(layer, block)
        if layer > 0:
            for copy in outgoing:
                copy.wait_send()
            started[:] = [copy for copy in started if all(copy is not old for old in outgoing)]
        attention()
        outgoing = [
            send(
                o_s.at[ahead(o)],
                ag.at[layer, t, s],
                az_send.at[layer, o],
                az_recv.at[layer, o],
                {"sp": ahead(o)},
            )
            for o in hops
        ]
        if not last:
            qkv_fly = send_qkv(layer + 1)
        ag[layer, t, s] = o_s[s]
        out_ready = relay_out(layer, out_fly)
        for copy in outgoing:
            copy.wait_recv()
        block = ag.at[layer, t]
        across = send(block, block, at_send.at[layer, 0], at_recv.at[layer, 0], {"tp": side})
        beside = send(block, block, at_send.at[layer, 1], at_recv.at[layer, 1], {"tp": core})
        across.wait_recv()
        block = ag.at[layer, side]
        corner = send(block, block, at_send.at[layer, 2], at_recv.at[layer, 2], {"tp": core})
        for copy in out_ready:
            copy.wait_recv()
        beside.wait_recv()
        corner.wait_recv()
        heads_all = ag[layer].reshape(tps * seqs * head, rows)
        weight = wo[layer].reshape(-1, cols)
        product = lax.dot_general(
            heads_all,
            weight,
            (((0,), (0,)), ((), ())),
            preferred_element_type=jnp.float32,
        )
        kept = xg[layer, t, block_rows(s), :].astype(jnp.float32)
        fresh = (kept + product).astype(jnp.bfloat16)
        if not last:
            xg[layer + 1, t, block_rows(s), :] = fresh
            for way in (0, 1):
                start_onward(layer + 1, way, 0)
            project_ready = relay_qkv(layer + 1, qkv_fly)
            out_fly = send_out(layer + 1)
        else:
            fin[t] = fresh
            cuts = fn_send.shape[0]
            tall = rows // cuts
            crossing, beside = [], []
            for c in range(cuts):
                part = fin.at[t, pl.ds(c * tall, tall), :]
                crossing.append(send(part, part, fn_send.at[c, 0], fn_recv.at[c, 0], {"tp": side}))
                beside.append(send(part, part, fn_send.at[c, 1], fn_recv.at[c, 1], {"tp": core}))
            for c in range(cuts):
                crossing[c].wait_recv()
                part = fin.at[side, pl.ds(c * tall, tall), :]
                beside.append(send(part, part, fn_send.at[c, 2], fn_recv.at[c, 2], {"tp": core}))
            for copy in beside:
                copy.wait_recv()
            for part in range(tps):
                out_ref[:, part * cols : (part + 1) * cols] = fin[part]
    for copy in started:
        copy.wait_send()
    for layer in range(layers):
        for o in range(1 if layer == 0 else 0, seqs):
            for kind in range(3):
                tp_copy(layer, kind, ahead(o)).wait_send()
        for way in (0, 1):
            for k in range(seqs - 1):
                copy, valid = onward(layer, way, k)

                @pl.when(valid)
                def _(copy=copy):
                    copy.wait_send()


def fused_device(
    sizes,
    stream,
    doc_ids,
    norm_gain,
    query_weight,
    key_weight,
    value_weight,
    out_weight,
    query_gain,
    key_gain,
    rel_bias,
):
    groups, seqs, tps = sizes
    rows, width = stream.shape
    cols = width // tps
    layers, deep, _ = query_weight.shape
    head = query_gain.shape[1]
    depth = -(-LEFT * SEG // rows)

    padded = jnp.pad(
        rel_bias, ((0, 0), (0, (depth + 2) * rows - rel_bias.shape[1])), mode="edge"
    )
    docs8 = jnp.broadcast_to(doc_ids.astype(jnp.float32)[None], (8, rows))
    dma = pltpu.SemaphoreType.DMA
    bf16 = jnp.bfloat16
    scratch = [
        pltpu.VMEM((layers, seqs, 3 * head, deep), bf16),
        pltpu.VMEM((layers, tps, seqs * rows, cols), bf16),
        pltpu.VMEM((layers, seqs, 3 * head, deep), bf16),
        pltpu.VMEM((layers, seqs) + out_weight.shape[1:], bf16),
        pltpu.VMEM((seqs, 8, rows), jnp.float32),
        pltpu.VMEM((seqs, rows, 128), jnp.float32),
        pltpu.VMEM((layers, tps, seqs, head, rows), bf16),
        pltpu.VMEM((tps, rows, cols), bf16),
        pltpu.VMEM((depth + 1, rows, rows), jnp.float32),
        pltpu.VMEM((rows, width), bf16),
        pltpu.VMEM((seqs, head, rows), bf16),
        pltpu.VMEM((seqs, rows, head), bf16),
        pltpu.VMEM((seqs, head, rows), bf16),
        pltpu.VMEM((seqs, head, rows), bf16),
    ]
    scratch += [dma((seqs,))] * 2 + [dma((layers, 2, seqs))] * 2 + [dma((layers, seqs))] * 14
    scratch += [dma((layers, seqs))] * 2 + [dma((layers, 3))] * 2 + [dma((2, 3))] * 2
    return pl.pallas_call(
        functools.partial(fused_kernel, sizes),
        name="fused_layers",
        out_shape=jax.ShapeDtypeStruct((rows, width), bf16),
        in_specs=[pl.BlockSpec(memory_space=pltpu.VMEM)] * 10,
        out_specs=pl.BlockSpec(memory_space=pltpu.VMEM),
        scratch_shapes=scratch,
        compiler_params=pltpu.CompilerParams(
            collective_id=0, has_side_effects=True, vmem_limit_bytes=60 * 1024 * 1024
        ),
    )(
        stream,
        docs8,
        norm_gain,
        query_weight,
        key_weight,
        value_weight,
        out_weight,
        query_gain,
        key_gain,
        padded,
    )


def solution(mesh):
    placed = (
        P(("grp", "sp"), None),
        P(("grp", "sp")),
        P(),
        P(None, "sp", "tp"),
        P(None, "sp", "tp"),
        P(None, "sp", "tp"),
        P(None, "sp", "tp"),
        P(),
        P(),
        P("tp", None),
    )
    sizes = tuple(mesh.shape[axis] for axis in ("grp", "sp", "tp"))

    def body(*args):
        one_head_each = args[-1].shape[0] == sizes[1]
        fits = sizes[0] == 2 and sizes[2] == 4 and args[0].shape[0] == MAXREL
        if one_head_each and fits:
            return fused_device(sizes, *args)
        return on_device(*args)

    return jax.shard_map(
        body, mesh=mesh, in_specs=placed, out_specs=P(("grp", "sp"), None), check_vma=False
    )
```

```python
import functools

import jax
import jax.numpy as jnp
from jax import lax
from jax.experimental import pallas as pl
from jax.experimental.pallas import tpu as pltpu
from jax.sharding import PartitionSpec as P

SEG = 64
LEFT = 8
MAXREL = 256
LAYERS = 2


epsilon = 1e-06


def shifted(value, axis, steps):
    count = lax.axis_size(axis)
    initial, last = (max(0, -steps), min(count, count - steps))
    return lax.ppermute(value, axis, [(source, source + steps) for source in range(initial, last)])


def row_norm(values, gain):
    return values * lax.rsqrt(jnp.mean(values * values, axis=-1, keepdims=True) + epsilon) * gain


def bias_table(rel_bias):
    heads_here = rel_bias.shape[0]
    reach = LEFT * SEG
    width = (LEFT + 1) * SEG
    highest = reach + SEG - 1
    reversed_bias = rel_bias[:, ::-1]
    upper_fill = jnp.broadcast_to(rel_bias[:, -1:], (heads_here, highest - MAXREL))
    flat_row = jnp.concatenate([upper_fill, reversed_bias[:, : MAXREL + SEG]], axis=1)
    lines = [
        flat_row[:, SEG - 1 - position : SEG - 1 - position + width] for position in range(SEG)
    ]
    return jnp.stack(lines, axis=1)


def attend(query, ext_keys, ext_values, ext_docs, own_docs, offset, table):
    rows, heads_here, head_size = query.shape
    count = rows // SEG
    width = (LEFT + 1) * SEG
    blocks = query.reshape(count, SEG, heads_here, head_size)
    key_blocks = ext_keys.reshape(count + LEFT, SEG, heads_here, head_size)
    value_blocks = ext_values.reshape(count + LEFT, SEG, heads_here, head_size)
    doc_blocks = ext_docs.reshape(count + LEFT, SEG)
    score_parts = [
        jnp.einsum(
            "nqhd,nkhd->nhqk",
            blocks,
            key_blocks[earlier : earlier + count],
            preferred_element_type=jnp.float32,
        )
        for earlier in range(LEFT + 1)
    ]
    scores = jnp.concatenate(score_parts, axis=-1)
    scores = scores * head_size ** (-0.5) + table[None]
    doc_band = jnp.concatenate(
        [doc_blocks[earlier : earlier + count] for earlier in range(LEFT + 1)], axis=1
    )
    key_pos = (
        offset
        + SEG * jnp.arange(count, dtype=jnp.int32)[:, None]
        - LEFT * SEG
        + jnp.arange(width, dtype=jnp.int32)[None, :]
    )
    allowed = (key_pos >= 0)[:, None, None, :] & (
        doc_band[:, None, None, :] == own_docs.reshape(count, SEG)[:, None, :, None]
    )
    scores = jnp.where(allowed, scores, -1e30)
    peak = jnp.max(scores, axis=-1, keepdims=True)
    expo = jnp.exp(scores - peak)
    weights = (expo / jnp.sum(expo, axis=-1, keepdims=True)).astype(jnp.bfloat16)
    mixed = jnp.zeros((count, SEG, heads_here, head_size), jnp.float32)
    for earlier in range(LEFT + 1):
        part_weights = weights[..., earlier * SEG : (earlier + 1) * SEG]
        mixed = mixed + jnp.einsum(
            "nhqk,nkhd->nqhd",
            part_weights,
            value_blocks[earlier : earlier + count],
            preferred_element_type=jnp.float32,
        )
    return mixed.astype(jnp.bfloat16).reshape(rows, heads_here * head_size)


def on_device(
    stream,
    doc_ids,
    norm_gain,
    query_weight,
    key_weight,
    value_weight,
    out_weight,
    query_gain,
    key_gain,
    rel_bias,
):
    rows = stream.shape[0]
    heads_here = rel_bias.shape[0]
    head_size = query_gain.shape[1]
    local_width = heads_here * head_size
    reach = LEFT * SEG
    depth = -(-reach // rows)
    offset = lax.axis_index("sp") * rows
    col_width = out_weight.shape[2]
    col_start = lax.axis_index("tp") * col_width
    table = bias_table(rel_bias)
    x = stream
    for layer in range(LAYERS):
        widened = x.astype(jnp.float32)
        normed = row_norm(widened, norm_gain[layer]).astype(jnp.bfloat16)
        own_cols = normed
        q_raw = jnp.dot(
            own_cols,
            lax.all_gather(query_weight[layer], "sp", axis=0, tiled=True),
            preferred_element_type=jnp.float32,
        )
        k_raw = jnp.dot(
            normed,
            lax.all_gather(key_weight[layer], "sp", axis=0, tiled=True),
            preferred_element_type=jnp.float32,
        )
        v_raw = jnp.dot(
            normed,
            lax.all_gather(value_weight[layer], "sp", axis=0, tiled=True),
            preferred_element_type=jnp.float32,
        )
        query = row_norm(q_raw.reshape(rows, heads_here, head_size), query_gain[layer]).astype(
            jnp.bfloat16
        )
        keys = row_norm(
            k_raw.reshape(normed.shape[0], heads_here, head_size), key_gain[layer]
        ).astype(jnp.bfloat16)
        values = v_raw.astype(jnp.bfloat16)
        flat_keys = keys.reshape(rows, local_width)
        tail = (flat_keys, values, doc_ids)
        received = [
            shifted((tail[0], tail[1], tail[2]), "sp", distance_back)
            for distance_back in range(depth, 0, -1)
        ]
        ext_keys = jnp.concatenate([item[0] for item in received] + [flat_keys], axis=0)
        ext_values = jnp.concatenate([item[1] for item in received] + [values], axis=0)
        ext_docs = jnp.concatenate([item[2] for item in received] + [doc_ids], axis=0)
        ext_keys = ext_keys.reshape(reach + rows, heads_here, head_size)
        ext_values = ext_values.reshape(reach + rows, heads_here, head_size)
        attended = attend(query, ext_keys, ext_values, ext_docs, doc_ids, offset, table)
        all_heads = lax.all_gather(attended, "tp", axis=1, tiled=True)
        projected = jnp.dot(
            all_heads,
            lax.all_gather(out_weight[layer], "sp", axis=0, tiled=True),
            preferred_element_type=jnp.float32,
        )
        own_cols = lax.dynamic_slice_in_dim(widened, col_start, col_width, 1)
        new_cols = (own_cols + projected).astype(jnp.bfloat16)
        x = lax.all_gather(new_cols, "tp", axis=1, tiled=True)
    return x


MESH = pl.DeviceIdType.MESH
NEG = -1e30


def fused_kernel(
    sizes,
    x_ref,
    docs_ref,
    ngain_ref,
    qw_ref,
    kw_ref,
    vw_ref,
    woin_ref,
    qgain_ref,
    kgain_ref,
    bias_ref,
    out_ref,
    wt_ref,
    xg,
    wq,
    wo,
    docs,
    dcol,
    ag,
    fin,
    bias,
    nb,
    q_s,
    k_s,
    v_s,
    o_s,
    doc_send,
    doc_recv,
    xz_send,
    xz_recv,
    xa_send,
    xa_recv,
    xb_send,
    xb_recv,
    xc_send,
    xc_recv,
    wz_send,
    wz_recv,
    wy_send,
    wy_recv,
    oz_send,
    oz_recv,
    oy_send,
    oy_recv,
    az_send,
    az_recv,
    at_send,
    at_recv,
    fn_send,
    fn_recv,
):
    groups, seqs, tps = sizes
    rows, width = x_ref.shape
    cols = width // tps
    head = qgain_ref.shape[1]
    layers = wt_ref.shape[0]
    depth = bias.shape[0] - 1
    grp = lax.axis_index("grp")
    s = lax.axis_index("sp")
    t = lax.axis_index("tp")
    other_grp = 1 - grp
    core = t + 1 - 2 * lax.rem(t, 2)
    side = lax.rem(t + 2, tps)
    diag = core + 2 - 4 * (core // 2)
    started = []

    def send(src, dst, send_sem, recv_sem, where):
        copy = pltpu.make_async_remote_copy(
            src_ref=src,
            dst_ref=dst,
            send_sem=send_sem,
            recv_sem=recv_sem,
            device_id=where,
            device_id_type=MESH,
        )
        copy.start()
        started.append(copy)
        return copy

    def ahead(o):
        return lax.rem(s + o, seqs)

    def behind(o):
        return lax.rem(s + seqs - o, seqs)

    def block_rows(i):
        return pl.ds(pl.multiple_of(i * rows, rows), rows)

    barrier = pltpu.get_barrier_semaphore()
    partners = [{"sp": ahead(o)} for o in range(1, seqs)]
    partners += [{"tp": core}, {"tp": side}, {"grp": other_grp}]
    for where in partners:
        pl.semaphore_signal(barrier, inc=1, device_id=where, device_id_type=MESH)
    pl.semaphore_wait(barrier, len(partners))

    own_cols = pl.ds(pl.multiple_of(t * cols, cols), cols)
    whalf = wt_ref.shape[2] // 2
    ohalf = woin_ref.shape[1] // 2
    wpart = pl.ds(pl.multiple_of(grp * whalf, whalf), whalf)
    opart = pl.ds(pl.multiple_of(grp * ohalf, ohalf), ohalf)
    hops = list(range(1, seqs))

    doc_c = [
        send(docs_ref, docs.at[s], doc_send.at[o], doc_recv.at[o], {"sp": ahead(o)}) for o in hops
    ]
    def passing(layer, way, k, arriving):
        block = s - k if way == 0 else s + k
        if arriving:
            block = block - 1 if way == 0 else block + 1
        inside = block >= 0 if way == 0 else block < seqs
        return block, inside

    def onward(layer, way, k):
        block, inside = passing(layer, way, k, False)
        open_end = s < seqs - 1 if way == 0 else s > 0
        place = xg.at[layer, t, block_rows(block), :]
        copy = pltpu.make_async_remote_copy(
            src_ref=x_ref.at[:, own_cols] if layer == 0 and k == 0 else place,
            dst_ref=place,
            send_sem=xz_send.at[layer, way, k],
            recv_sem=xz_recv.at[layer, way, k],
            device_id={"sp": s + 1 if way == 0 else s - 1},
            device_id_type=MESH,
        )
        return copy, inside & open_end

    def start_onward(layer, way, k):
        copy, valid = onward(layer, way, k)

        @pl.when(valid)
        def _():
            copy.start()

    def tp_copy(layer, kind, block):
        held = side if kind == 2 else t
        place = xg.at[layer, held, block_rows(block), :]
        send_sem, recv_sem = ((xa_send, xa_recv), (xb_send, xb_recv), (xc_send, xc_recv))[kind]
        return pltpu.make_async_remote_copy(
            src_ref=place,
            dst_ref=place,
            send_sem=send_sem.at[layer, block],
            recv_sem=recv_sem.at[layer, block],
            device_id={"tp": side if kind == 1 else core},
            device_id_type=MESH,
        )

    for way in (0, 1):
        start_onward(0, way, 0)

    def send_qkv(layer):
        return {
            o: send(
                wt_ref.at[layer, ahead(o), wpart, :],
                wq.at[layer, s, wpart, :],
                wz_send.at[layer, o],
                wz_recv.at[layer, o],
                {"sp": ahead(o)},
            )
            for o in hops
        }

    def send_out(layer):
        return {
            o: send(
                woin_ref.at[layer, opart, :],
                wo.at[layer, s, opart, :],
                oz_send.at[layer, o],
                oz_recv.at[layer, o],
                {"sp": ahead(o)},
            )
            for o in hops
        }

    def relay_qkv(layer, flying):
        result = []
        for o in hops:
            flying[o].wait_recv()
            block = wq.at[layer, behind(o), wpart, :]
            result.append(
                send(block, block, wy_send.at[layer, o], wy_recv.at[layer, o], {"grp": other_grp})
            )
        return result

    def relay_out(layer, flying):
        result = []
        for o in hops:
            flying[o].wait_recv()
            block = wo.at[layer, behind(o), opart, :]
            result.append(
                send(block, block, oy_send.at[layer, o], oy_recv.at[layer, o], {"grp": other_grp})
            )
        return result

    for part in range(tps):
        xg[0, part, block_rows(s), :] = x_ref[:, part * cols : (part + 1) * cols]
    for layer in range(layers):
        for which, source in enumerate((qw_ref, kw_ref, vw_ref)):
            turned = jnp.transpose(source[layer])
            for i in range(seqs):
                wt_ref[layer, i, which * head : (which + 1) * head, :] = turned[
                    i * head : (i + 1) * head, :
                ]
        wo[layer, s] = woin_ref[layer]
        wq[layer, s] = wt_ref[layer, s]
    docs[s] = docs_ref[...]
    key_seg = lax.broadcasted_iota(jnp.int32, (rows, rows), 0) // SEG
    query_seg = lax.broadcasted_iota(jnp.int32, (rows, rows), 1) // SEG
    for d in range(depth + 1):
        spread = jnp.broadcast_to(
            bias_ref[pl.ds(s, 1), d * rows : (d + 2) * rows], (rows, 2 * rows)
        )
        rolled = pltpu.roll(spread, 0, 1, stride=1, stride_axis=0)
        gap = query_seg + (d * rows) // SEG - key_seg
        bias[d] = jnp.where((gap >= 0) & (gap <= LEFT), rolled[:, rows:], NEG)
    for copy in doc_c:
        copy.wait_recv()
    for i in range(seqs):
        dcol[i] = jnp.transpose(jnp.broadcast_to(docs[i, 0:1, :], (128, rows)))

    def fan(layer, block):
        tp_copy(layer, 1, block).start()
        tp_copy(layer, 0, block).start()

    def pass_on(layer, block):
        tp_copy(layer, 1, block).wait_recv()
        tp_copy(layer, 2, block).start()

    def spread_tp(layer, own_too):
        fetched = None
        if own_too:
            fan(layer, s)
        for k in range(seqs - 1):
            for way in (0, 1):
                block, inside = passing(layer, way, k, True)

                @pl.when(inside)
                def _(block=block, way=way, k=k):
                    onward(layer, way, k)[0].wait_recv()
                    if k + 1 < seqs - 1:
                        start_onward(layer, way, k + 1)
                    fan(layer, block)

            if k == 0 and own_too:
                fetched = relay_qkv(layer, qkv_fly)
                pass_on(layer, s)
            if k == min(1, seqs - 2) and not own_too:
                flying = send_qkv(layer)
            pass_slots(layer, k - 1)
        out_flying = None
        if own_too:
            out_flying = send_out(layer)
        pass_slots(layer, seqs - 2)
        if not own_too:
            fetched = relay_qkv(layer, flying)
            out_flying = send_out(layer)
        return fetched, out_flying

    def pass_slots(layer, k):
        if k < 0:
            return
        for way in (0, 1):
            block, inside = passing(layer, way, k, True)

            @pl.when(inside)
            def _(block=block):
                pass_on(layer, block)

    def nth(v):
        orders = [
            sorted((b for b in range(seqs) if b != c), key=lambda b: abs(b - c))
            for c in range(seqs)
        ]
        block = orders[0][v - 1]
        for c in range(1, seqs):
            block = jnp.where(s == c, orders[c][v - 1], block)
        return block

    def project(layer, i):
        total = jnp.zeros((rows, 1), jnp.float32)
        for part in range(tps):
            piece = xg[layer, part, block_rows(i), :].astype(jnp.float32)
            total = total + jnp.sum(piece * piece, axis=1, keepdims=True)
        factor = lax.rsqrt(total * (1.0 / width) + epsilon)
        for part in range(tps):
            piece = xg[layer, part, block_rows(i), :].astype(jnp.float32)
            gain = ngain_ref[layer : layer + 1, part * cols : (part + 1) * cols]
            nb[:, part * cols : (part + 1) * cols] = (piece * factor * gain).astype(jnp.bfloat16)
        span = width // seqs
        raw = jnp.zeros((3 * head, rows), jnp.float32)
        for part in range(seqs):
            raw = raw + lax.dot_general(
                wq[layer, part],
                nb[:, part * span : (part + 1) * span],
                (((1,), (1,)), ((), ())),
                preferred_element_type=jnp.float32,
            )

        def normal(value, gain):
            mean = jnp.mean(value * value, axis=0, keepdims=True)
            column = jnp.transpose(jnp.broadcast_to(gain, (128, head)))[:, 0:1]
            return value * lax.rsqrt(mean + epsilon) * column

        q_s[i] = (normal(raw[:head], qgain_ref[layer : layer + 1, :]) * head ** (-0.5)).astype(jnp.bfloat16)
        k_s[i] = jnp.transpose(normal(raw[head : 2 * head], kgain_ref[layer : layer + 1, :])).astype(jnp.bfloat16)
        v_s[i] = raw[2 * head :].astype(jnp.bfloat16)

    def attention():
        for j in range(seqs):
            pieces = []
            for i in range(max(0, j - depth), j + 1):
                score = jnp.dot(k_s[i], q_s[j], preferred_element_type=jnp.float32)
                same = dcol[i][:, 0:1] == docs[j, 0:1, :]
                pieces.append((i, jnp.where(same, score + bias[j - i], NEG)))
            peak = pieces[0][1].max(axis=0, keepdims=True)
            for _, piece in pieces[1:]:
                peak = jnp.maximum(peak, piece.max(axis=0, keepdims=True))
            mass = jnp.zeros((1, rows), jnp.float32)
            mixed = jnp.zeros((head, rows), jnp.float32)
            for i, piece in pieces:
                expo = jnp.exp(piece - peak)
                mass = mass + jnp.sum(expo, axis=0, keepdims=True)
                mixed = mixed + jnp.dot(
                    v_s[i], expo.astype(jnp.bfloat16), preferred_element_type=jnp.float32
                )
            o_s[lax.rem(j, seqs)] = (mixed / mass).astype(jnp.bfloat16)

    for layer in range(layers):
        last = layer == layers - 1
        project_ready, out_fly = spread_tp(layer, layer > 0)
        for copy in project_ready:
            copy.wait_recv()
        for v in range(seqs):
            block = nth(v) if v else s
            if v or layer > 0:
                tp_copy(layer, 0, block).wait_recv()
                tp_copy(layer, 2, block).wait_recv()
            project(layer, block)
        if layer > 0:
            for copy in outgoing:
                copy.wait_send()
            started[:] = [copy for copy in started if all(copy is not old for old in outgoing)]
        attention()
        outgoing = [
            send(
                o_s.at[ahead(o)],
                ag.at[layer, t, s],
                az_send.at[layer, o],
                az_recv.at[layer, o],
                {"sp": ahead(o)},
            )
            for o in hops
        ]
        if not last:
            qkv_fly = send_qkv(layer + 1)
        ag[layer, t, s] = o_s[s]
        out_ready = relay_out(layer, out_fly)
        for copy in outgoing:
            copy.wait_recv()
        block = ag.at[layer, t]
        across = send(block, block, at_send.at[layer, 0], at_recv.at[layer, 0], {"tp": side})
        beside = send(block, block, at_send.at[layer, 1], at_recv.at[layer, 1], {"tp": core})
        across.wait_recv()
        block = ag.at[layer, side]
        corner = send(block, block, at_send.at[layer, 2], at_recv.at[layer, 2], {"tp": core})
        for copy in out_ready:
            copy.wait_recv()
        beside.wait_recv()
        corner.wait_recv()
        heads_all = ag[layer].reshape(tps * seqs * head, rows)
        weight = wo[layer].reshape(-1, cols)
        product = lax.dot_general(
            heads_all,
            weight,
            (((0,), (0,)), ((), ())),
            preferred_element_type=jnp.float32,
        )
        kept = xg[layer, t, block_rows(s), :].astype(jnp.float32)
        fresh = (kept + product).astype(jnp.bfloat16)
        if not last:
            xg[layer + 1, t, block_rows(s), :] = fresh
            for way in (0, 1):
                start_onward(layer + 1, way, 0)
        else:
            fin[t] = fresh
            cuts = fn_send.shape[0]
            tall = rows // cuts
            crossing, beside = [], []
            for c in range(cuts):
                part = fin.at[t, pl.ds(c * tall, tall), :]
                crossing.append(send(part, part, fn_send.at[c, 0], fn_recv.at[c, 0], {"tp": side}))
                beside.append(send(part, part, fn_send.at[c, 1], fn_recv.at[c, 1], {"tp": core}))
            for c in range(cuts):
                crossing[c].wait_recv()
                part = fin.at[side, pl.ds(c * tall, tall), :]
                beside.append(send(part, part, fn_send.at[c, 2], fn_recv.at[c, 2], {"tp": core}))
            for copy in beside:
                copy.wait_recv()
            for part in range(tps):
                out_ref[:, part * cols : (part + 1) * cols] = fin[part]
    for copy in started:
        copy.wait_send()
    for layer in range(layers):
        for o in range(1 if layer == 0 else 0, seqs):
            for kind in range(3):
                tp_copy(layer, kind, ahead(o)).wait_send()
        for way in (0, 1):
            for k in range(seqs - 1):
                copy, valid = onward(layer, way, k)

                @pl.when(valid)
                def _(copy=copy):
                    copy.wait_send()


def fused_device(
    sizes,
    stream,
    doc_ids,
    norm_gain,
    query_weight,
    key_weight,
    value_weight,
    out_weight,
    query_gain,
    key_gain,
    rel_bias,
):
    groups, seqs, tps = sizes
    rows, width = stream.shape
    cols = width // tps
    layers, deep, _ = query_weight.shape
    head = query_gain.shape[1]
    depth = -(-LEFT * SEG // rows)

    padded = jnp.pad(
        rel_bias, ((0, 0), (0, (depth + 2) * rows - rel_bias.shape[1])), mode="edge"
    )
    docs8 = jnp.broadcast_to(doc_ids.astype(jnp.float32)[None], (8, rows))
    dma = pltpu.SemaphoreType.DMA
    bf16 = jnp.bfloat16
    scratch = [
        pltpu.VMEM((layers, seqs, 3 * head, deep), bf16),
        pltpu.VMEM((layers, tps, seqs * rows, cols), bf16),
        pltpu.VMEM((layers, seqs, 3 * head, deep), bf16),
        pltpu.VMEM((layers, seqs) + out_weight.shape[1:], bf16),
        pltpu.VMEM((seqs, 8, rows), jnp.float32),
        pltpu.VMEM((seqs, rows, 128), jnp.float32),
        pltpu.VMEM((layers, tps, seqs, head, rows), bf16),
        pltpu.VMEM((tps, rows, cols), bf16),
        pltpu.VMEM((depth + 1, rows, rows), jnp.float32),
        pltpu.VMEM((rows, width), bf16),
        pltpu.VMEM((seqs, head, rows), bf16),
        pltpu.VMEM((seqs, rows, head), bf16),
        pltpu.VMEM((seqs, head, rows), bf16),
        pltpu.VMEM((seqs, head, rows), bf16),
    ]
    scratch += [dma((seqs,))] * 2 + [dma((layers, 2, seqs))] * 2 + [dma((layers, seqs))] * 14
    scratch += [dma((layers, seqs))] * 2 + [dma((layers, 3))] * 2 + [dma((2, 3))] * 2
    return pl.pallas_call(
        functools.partial(fused_kernel, sizes),
        name="fused_layers",
        out_shape=jax.ShapeDtypeStruct((rows, width), bf16),
        in_specs=[pl.BlockSpec(memory_space=pltpu.VMEM)] * 10,
        out_specs=pl.BlockSpec(memory_space=pltpu.VMEM),
        scratch_shapes=scratch,
        compiler_params=pltpu.CompilerParams(
            collective_id=0, has_side_effects=True, vmem_limit_bytes=60 * 1024 * 1024
        ),
    )(
        stream,
        docs8,
        norm_gain,
        query_weight,
        key_weight,
        value_weight,
        out_weight,
        query_gain,
        key_gain,
        padded,
    )


def solution(mesh):
    placed = (
        P(("grp", "sp"), None),
        P(("grp", "sp")),
        P(),
        P(None, "sp", "tp"),
        P(None, "sp", "tp"),
        P(None, "sp", "tp"),
        P(None, "sp", "tp"),
        P(),
        P(),
        P("tp", None),
    )
    sizes = tuple(mesh.shape[axis] for axis in ("grp", "sp", "tp"))

    def body(*args):
        one_head_each = args[-1].shape[0] == sizes[1]
        fits = sizes[0] == 2 and sizes[2] == 4 and args[0].shape[0] == MAXREL
        if one_head_each and fits:
            return fused_device(sizes, *args)
        return on_device(*args)

    return jax.shard_map(
        body, mesh=mesh, in_specs=placed, out_specs=P(("grp", "sp"), None), check_vma=False
    )
```
